32 devices in a mesh: fs: 4 (over z), rep: 4 (over y, x), tp: 2 (over core).
Axes of the slice: x: 2, y: 2, z: 4, core: 2. Of those that a mesh axis runs over, the one named last changes fastest.
Arguments:
- input_act: bfloat16 [12288, 2048], P(('fs', 'rep')), may hold values from -6 to 6
- query_cot: bfloat16 [12288, 1024], P(('fs', 'rep'), 'tp'), may hold values from -6 to 6
- out_cot: bfloat16 [12288, 2048], P(('fs', 'rep')), may hold values from -6 to 6
- attn_out: bfloat16 [12288, 1024], P(('fs', 'rep'), 'tp'), may hold values from -6 to 6
- query_w: float32 [2048, 1024], P('fs', 'tp'), may hold values from -0.125 to 0.125
- out_w: float32 [1024, 2048], P('tp', 'fs'), may hold values from -0.1875 to 0.1875
- query_factor: bfloat16 [2048, 512], P('fs'), may hold values from -0.125 to 0.125
- out_factor: bfloat16 [2048, 512], P('fs'), may hold values from -0.125 to 0.125
- first_q: float32 [512, 1024], P('fs', 'tp'), may hold values from -6 to 6
- second_q: float32 [512, 1024], P('fs', 'tp'), may hold values from 0.075 to 120
- first_o: float32 [512, 1024], P('fs', 'tp'), may hold values from -6 to 6
- second_o: float32 [512, 1024], P('fs', 'tp'), may hold values from 0.075 to 120
Outputs:
- new_query_w: float32 [2048, 1024], P('fs', 'tp')
- new_out_w: float32 [1024, 2048], P('tp', 'fs')
- query_step: float32 [2048, 1024], P('fs', 'tp')
- out_step: float32 [1024, 2048], P('tp', 'fs')
- new_first_q: float32 [512, 1024], P('fs', 'tp')
- new_second_q: float32 [512, 1024], P('fs', 'tp')
- new_first_o: float32 [512, 1024], P('fs', 'tp')
- new_second_o: float32 [512, 1024], P('fs', 'tp')
- query_copy: bfloat16 [2048, 1024], P(None, 'tp')
- out_copy: bfloat16 [1024, 2048], P('tp')
The draws below stay inside these ranges and needn't reach their ends.
All inputs are finite; a program needn't handle non-finite values.
Results may differ from the reference program's by a relative error of at most 0.0085.
Values may be sent and summed in bfloat16 or wider, within the bound.
A program may use at most 64 MiB of HBM per device.

```python
import math
import jax
import jax.numpy as jnp
from jax import lax

D = 2048
RANK = 512
HQ = 1024
TOKENS = 12288


def second_law(key, marker):
    local_key = jax.random.fold_in(key, marker)
    row_place = jnp.arange(RANK, dtype=jnp.float32)[:, None] / RANK
    spread = jax.random.uniform(local_key, (RANK, HQ), jnp.float32, math.log(0.3), math.log(3.0))
    return jnp.exp(spread + row_place * math.log(10.0))


def draw_second_q(key, part):
    return second_law(key, 11)


def draw_second_o(key, part):
    return second_law(key, 23)


def raised(values, stream_key, source, target, shards_of, factor):
    def block_of(position):
        return (jnp.arange(values.shape[position]) // (values.shape[position] // shards_of)).reshape((-1,) + (1,) * (values.ndim - 1 - position))

    near = jax.random.permutation(stream_key, shards_of)[block_of(target)]
    far = (block_of(target) + shards_of // 2) % shards_of
    return jnp.where((block_of(source) == near) | (block_of(source) == far), factor * values, values)


def level_of(own_key, shape, shards, least, high):
    factor_of, own = 1.0, jax.random.fold_in(own_key, 6)
    for position, parts in shards:
        steps = jnp.exp(jax.random.uniform(jax.random.fold_in(own, position), (parts,), jnp.float32, least / len(shards), high / len(shards)))
        factor_of = factor_of * jnp.repeat(steps, shape[position] // parts).reshape([-1 if axis == position else 1 for axis in range(len(shape))])
    return factor_of


def normal_values(own_key, extent, width, reach, cuts=(), kind=jnp.bfloat16):
    values = jax.random.normal(own_key, extent, jnp.float32) * width
    if len(cuts) > 0:
        values = level_of(own_key, extent, cuts, -0.22, 0.18) * values
    return jnp.clip(values, min=-reach, max=reach).astype(kind)


def gaussian_with(stream_key, dims, width, bound, shards, heavy, kind=jnp.bfloat16):
    values = width * jax.random.normal(stream_key, dims, jnp.float32)
    if shards:
        values = values * level_of(stream_key, dims, shards, -0.22, 0.18)
    return jnp.clip(raised(values, jax.random.fold_in(stream_key, 3), *heavy), -bound, bound).astype(kind)


def setup_inputs(seed: int = 0) -> dict:
    key_of = jax.random.split(jax.random.key(seed), 13)
    input_act = gaussian_with(key_of[0], (TOKENS, D), 1.0, 6.0, ((0, 16),), (0, 1, 16, 2.0))
    query_cot = normal_values(key_of[1], (TOKENS, HQ), 1.0, 6.0, ((0, 16), (1, 2)))
    out_cot = gaussian_with(key_of[2], (TOKENS, D), 1.0, 6.0, ((0, 16),), (0, 1, 16, 2.0))
    attn_out = normal_values(key_of[3], (TOKENS, HQ), 1.0, 6.0, ((0, 16), (1, 2)))
    query_w = normal_values(key_of[4], (D, HQ), D ** -0.5, 0.125, ((0, 4), (1, 2)), jnp.float32)
    out_w = normal_values(key_of[5], (HQ, D), HQ ** -0.5, 0.1875, ((0, 2), (1, 4)), jnp.float32)
    query_factor = normal_values(key_of[6], (D, RANK), D ** -0.5, 0.125, ((0, 4),))
    out_factor = normal_values(key_of[7], (D, RANK), D ** -0.5, 0.125, ((0, 4),))
    first_q = normal_values(key_of[8], (RANK, HQ), 1.0, 6.0, ((0, 4), (1, 2)), jnp.float32)
    second_q = draw_second_q(jax.random.fold_in(key_of[12], 71), 0)
    first_o = normal_values(key_of[10], (RANK, HQ), 1.0, 6.0, ((0, 4), (1, 2)), jnp.float32)
    second_o = draw_second_o(jax.random.fold_in(key_of[12], 71), 0)
    return dict(input_act=input_act, query_cot=query_cot, out_cot=out_cot, attn_out=attn_out, query_w=query_w, out_w=out_w, query_factor=query_factor, out_factor=out_factor, first_q=first_q, second_q=second_q, first_o=first_o, second_o=second_o)


def contract_rows(left_side, right_side):
    return lax.dot_general(left_side, right_side, (((0,), (0,)), ((), ())), preferred_element_type=jnp.float32)

def exact_dot(left_side, right_side):
    return jnp.dot(left_side, right_side, precision=lax.Precision.HIGHEST, preferred_element_type=jnp.float32)

def reference(input_act, query_cot, out_cot, attn_out, query_w, out_w, query_factor, out_factor, first_q, second_q, first_o, second_o):
    scale_tokens = 1.0 / math.sqrt(TOKENS)
    grad_q = contract_rows(input_act, query_cot) * scale_tokens
    grad_o = contract_rows(out_cot, attn_out) * scale_tokens
    factor_q = query_factor.astype(jnp.float32)
    factor_o = out_factor.astype(jnp.float32)
    proj_q = exact_dot(factor_q.T, grad_q)
    proj_o = exact_dot(factor_o.T, grad_o)
    new_first_q = 0.8 * first_q + 0.2 * proj_q
    new_second_q = 0.9 * second_q + 0.1 * proj_q * proj_q
    new_first_o = 0.8 * first_o + 0.2 * proj_o
    new_second_o = 0.9 * second_o + 0.1 * proj_o * proj_o
    dir_q = new_first_q / jnp.sqrt(new_second_q)
    dir_o = new_first_o / jnp.sqrt(new_second_o)
    mean_square = (jnp.sum(dir_q * dir_q) + jnp.sum(dir_o * dir_o)) / (2 * RANK * HQ)
    norm_scale = jnp.sqrt(mean_square + 1e-06)
    query_step = exact_dot(factor_q, dir_q) / norm_scale
    out_step = (exact_dot(factor_o, dir_o) / norm_scale).T
    new_query_w = query_w - 0.01 * query_step
    new_out_w = out_w - 0.01 * out_step
    query_copy = new_query_w.astype(jnp.bfloat16)
    out_copy = new_out_w.astype(jnp.bfloat16)
    return (new_query_w, new_out_w, query_step, out_step, new_first_q, new_second_q, new_first_o, new_second_o, query_copy, out_copy)
```

```python
import functools
import math

import jax
import jax.numpy as jnp
from jax import lax
from jax.experimental import pallas as pl
from jax.experimental.pallas import tpu as pltpu
from jax.sharding import PartitionSpec as P

MESH = pl.DeviceIdType.MESH
F32 = jnp.float32
BF16 = jnp.bfloat16


def rcopy(src, dst, sems, index, there, **where):
    return pltpu.make_async_remote_copy(
        src_ref=src,
        dst_ref=dst,
        send_sem=sems[0].at[index],
        recv_sem=sems[1].at[there],
        device_id=where,
        device_id_type=MESH,
    )


def nt_dot(a, b):
    return lax.dot_general(a, b, (((1,), (1,)), ((), ())), preferred_element_type=F32)


def exchange_kernel(
    nf, nr, scale,
    x_ref, cq_ref, y_ref, ca_ref, wq_ref, wo_ref, fq_ref, fo_ref, m1q_ref, m2q_ref, m1o_ref, m2o_ref,
    fall_out, wq_out, wo_out, dir_out, proj_out, sq_out,
    acts, cots, cot_t, grads, fall, w32q, w32o, wbq, wbo, pieces, piece_in, summed, summed_in,
    moms, proj_all, dir_all, sq_buf,
    loc, fa_s, fa_r, fb_s, fb_r, fc_s, fc_r, wa_s, wa_r, wb_s, wb_r, ps_s, ps_r, ss_s, ss_r,
    pr_s, pr_r, da_s, da_r, db_s, db_r, sq_s, sq_r,
):
    f, r, t = lax.axis_index("fs"), lax.axis_index("rep"), lax.axis_index("tp")
    ot = 1 - t
    dl, rank = fq_ref.shape
    hl = cq_ref.shape[1]
    dq, hq = dl // nr, hl // nr
    rl = rank // nf
    pc = 2 * hl // nr
    ppa = nr // 2
    fa, fb, fc = (fa_s, fa_r), (fb_s, fb_r), (fc_s, fc_r)
    wa, wb = (wa_s, wa_r), (wb_s, wb_r)
    ps, ss, pr, da, db, sq = (ps_s, ps_r), (ss_s, ss_r), (pr_s, pr_r), (da_s, da_r), (db_s, db_r), (sq_s, sq_r)

    def fpeer(k):
        return lax.rem(f + k, nf)

    def rpeer(j):
        return lax.rem(r + j, nr)

    def each_f(body):
        lax.fori_loop(1, nf, lambda k, _: (body(k, fpeer(k)), 0)[1], 0)

    def rows(start, size):
        return pl.ds(pl.multiple_of(start, 16), size)

    def local(i, src, dst):
        return pltpu.make_async_copy(src, dst, loc.at[i])

    own_rows = rows(f * dl, dl)
    load_f = [local(0, fq_ref, fall.at[0, own_rows]), local(1, fo_ref, fall.at[1, own_rows])]
    load_w = [local(2, wq_ref, w32q), local(3, wo_ref, w32o)]
    load_c = [local(4, cq_ref, cots.at[0]), local(5, ca_ref, cots.at[1])]
    load_x = [local(6, x_ref, acts.at[0]), local(7, y_ref, acts.at[1])]
    for c in load_f + load_w + load_c + load_x:
        c.start()
    pcol = pl.ds(pl.multiple_of(lax.rem(r, ppa) * pc, pc), pc)

    @pl.when(r < ppa)
    def _():
        local(8, m1q_ref.at[:, pcol], moms.at[0]).start()
        local(9, m2q_ref.at[:, pcol], moms.at[1]).start()

    @pl.when(r >= ppa)
    def _():
        local(8, m1o_ref.at[:, pcol], moms.at[0]).start()
        local(9, m2o_ref.at[:, pcol], moms.at[1]).start()

    barrier = pltpu.get_barrier_semaphore()
    each_f(lambda k, p: pl.semaphore_signal(barrier, inc=1, device_id={"fs": p}, device_id_type=MESH))
    for j in range(1, nr):
        pl.semaphore_signal(barrier, inc=1, device_id={"rep": rpeer(j)}, device_id_type=MESH)
    pl.semaphore_signal(barrier, inc=1, device_id={"tp": ot}, device_id_type=MESH)
    pl.semaphore_wait(barrier, nf + nr - 1)

    def fchunk(core, block, part):
        ref = fall.at[core, rows(block * dl + part * dq, dq)]
        return ref

    def fa_copy(k, p):
        return rcopy(fchunk(t, f, r), fchunk(t, f, r), fa, p, f, fs=p)

    def fb_copy(p, j):
        return rcopy(fchunk(t, p, r), fchunk(t, p, r), fb, (p, rpeer(j)), (p, r), rep=rpeer(j))

    def fc_copy(p, part):
        return rcopy(fchunk(t, p, part), fchunk(t, p, part), fc, (p, part), (p, part), tp=ot)

    for c in load_f:
        c.wait()
    each_f(lambda k, p: fa_copy(k, p).start())

    for c in load_w:
        c.wait()
    wbq[...] = w32q[...].astype(BF16)
    wbo[...] = w32o[...].astype(BF16)
    keep_w = [local(2, wbq, wq_out.at[own_rows]), local(3, wbo, wo_out.at[f])]
    for c in keep_w:
        c.start()

    def wq_chunk(block):
        return wq_out.at[rows(block * dl + r * dq, dq)]

    def wo_chunk(block):
        return wo_out.at[block, rows(r * hq, hq)]

    def wa_copies(p):
        return (
            rcopy(wbq.at[rows(r * dq, dq)], wq_chunk(f), wa, (p, 0), (f, 0), fs=p),
            rcopy(wbo.at[rows(r * hq, hq)], wo_chunk(f), wa, (p, 1), (f, 1), fs=p),
        )

    def wa_recv(p):
        return (
            rcopy(wbq.at[rows(r * dq, dq)], wq_chunk(p), wa, (p, 0), (p, 0), fs=p),
            rcopy(wbo.at[rows(r * hq, hq)], wo_chunk(p), wa, (p, 1), (p, 1), fs=p),
        )

    def wb_copies(p, j):
        q = rpeer(j)
        return (
            rcopy(wq_chunk(p), wq_chunk(p), wb, (p, q, 0), (p, r, 0), rep=q),
            rcopy(wo_chunk(p), wo_chunk(p), wb, (p, q, 1), (p, r, 1), rep=q),
        )

    def wb_recv(p, j):
        q = rpeer(j)
        there_q = wq_out.at[rows(p * dl + q * dq, dq)]
        there_o = wo_out.at[p, rows(q * hq, hq)]
        return (
            rcopy(there_q, there_q, wb, (p, q, 0), (p, q, 0), rep=q),
            rcopy(there_o, there_o, wb, (p, q, 1), (p, q, 1), rep=q),
        )

    def start_all(copies):
        for c in copies:
            c.start()

    each_f(lambda k, p: start_all(wa_copies(p)))

    nb = min(512, x_ref.shape[1])

    def gradient(i):
        load_c[i].wait()
        cot_t[...] = cots[i].T
        load_x[i].wait()

        def column(n, _):
            cols = pl.ds(pl.multiple_of(n * nb, nb), nb)
            grads[i, :, cols] = jnp.dot(cot_t[...], acts[i, :, cols], preferred_element_type=F32).astype(BF16)
            return 0

        lax.fori_loop(0, x_ref.shape[1] // nb, column, 0)

    gradient(0)

    def forward_f(k, p):
        rcopy(fchunk(t, p, r), fchunk(t, p, r), fa, p, p, fs=p).wait_recv()
        for j in range(1, nr):
            fb_copy(p, j).start()
        fc_copy(p, r).start()

    each_f(forward_f)
    gradient(1)

    def across_f(k, p):
        for j in range(1, nr):
            q = rpeer(j)
            rcopy(fchunk(t, p, q), fchunk(t, p, q), fb, (p, q), (p, q), rep=q).wait_recv()
            fc_copy(p, q).start()

    each_f(across_f)

    def rest_f(k, p):
        for part in range(nr):
            rcopy(fchunk(ot, p, part), fchunk(ot, p, part), fc, (p, part), (p, part), tp=ot).wait_recv()

    each_f(rest_f)
    keep_f = local(0, fall, fall_out)
    keep_f.start()

    rb = min(256, rank)
    for i in range(2):
        def ranks(n, _, i=i):
            cols = pl.ds(pl.multiple_of(n * rb, rb), rb)
            term = jnp.dot(grads[i], fall[i, :, cols], preferred_element_type=F32).T.astype(BF16)
            for part in range(ppa):
                pieces[i * ppa + part, cols, :] = term[:, part * pc:(part + 1) * pc]
            return 0

        lax.fori_loop(0, rank // rb, ranks, 0)

    def ps_copy(j):
        q = rpeer(j)
        return rcopy(pieces.at[q], piece_in.at[r], ps, q, r, rep=q)

    for j in range(1, nr):
        ps_copy(j).start()

    def forward_w(k, p):
        for c in wa_recv(p):
            c.wait_recv()
        for j in range(1, nr):
            start_all(wb_copies(p, j))

    for j in range(1, nr):
        q = rpeer(j)
        rcopy(pieces.at[q], piece_in.at[q], ps, q, q, rep=q).wait_recv()
    total = pieces[r].astype(F32)
    for j in range(1, nr):
        total = total + piece_in[rpeer(j)].astype(F32)
    summed[...] = total.astype(BF16)

    def ss_copy(p):
        return rcopy(summed.at[rows(p * rl, rl)], summed_in.at[f], ss, p, f, fs=p)

    each_f(lambda k, p: ss_copy(p).start())
    each_f(forward_w)

    own_rank = rows(f * rl, rl)

    def gather_sum(k, total):
        p = fpeer(k)
        rcopy(summed.at[own_rank], summed_in.at[p], ss, p, p, fs=p).wait_recv()
        return total + summed_in[p].astype(F32)

    proj = lax.fori_loop(1, nf, gather_sum, summed[own_rank, :].astype(F32)).astype(BF16)
    proj_all[r] = proj

    def pr_copy(j):
        q = rpeer(j)
        return rcopy(proj_all.at[r], proj_all.at[r], pr, q, r, rep=q)

    proj = proj.astype(F32) * scale
    local(8, m1q_ref.at[:, pcol], moms.at[0]).wait()
    local(9, m2q_ref.at[:, pcol], moms.at[1]).wait()
    first = 0.8 * moms[0] + 0.2 * proj
    second = 0.9 * moms[1] + 0.1 * proj * proj
    dir_all[r, own_rank, :] = (first / jnp.sqrt(second)).astype(BF16)

    def da_copy(p):
        return rcopy(dir_all.at[r, own_rank], dir_all.at[r, own_rank], da, p, f, fs=p)

    each_f(lambda k, p: da_copy(p).start())
    for j in range(1, nr):
        pr_copy(j).start()

    def da_wait(k, p):
        there = dir_all.at[r, rows(p * rl, rl)]
        rcopy(there, there, da, p, p, fs=p).wait_recv()

    each_f(da_wait)

    def db_copy(j):
        q = rpeer(j)
        return rcopy(dir_all.at[r], dir_all.at[r], db, q, r, rep=q)

    for j in range(1, nr):
        db_copy(j).start()
    for j in range(1, nr):
        q = rpeer(j)
        rcopy(dir_all.at[q], dir_all.at[q], db, q, q, rep=q).wait_recv()
        rcopy(proj_all.at[q], proj_all.at[q], pr, q, q, rep=q).wait_recv()
    keep_d = [local(4, dir_all, dir_out), local(5, proj_all, proj_out)]
    start_all(keep_d)

    squares = jnp.zeros((8, pc), F32)
    for q in range(nr):
        d = dir_all[q].astype(F32)
        squares = squares + jnp.sum((d * d).reshape(rank // 8, 8, pc), axis=0)
    sq_buf[0] = squares
    sq_copy = rcopy(sq_buf.at[0], sq_buf.at[1], sq, 0, 0, tp=ot)
    sq_copy.start()
    sq_copy.wait_recv()
    sq_out[...] = jnp.zeros(sq_out.shape, F32) + jnp.sum(sq_buf[0] + sq_buf[1])

    def rest_w(k, p):
        for j in range(1, nr):
            for c in wb_recv(p, j):
                c.wait_recv()

    each_f(rest_w)

    def drain(k, p):
        fa_copy(k, p).wait_send()
        for c in wa_copies(p):
            c.wait_send()
        for j in range(1, nr):
            fb_copy(p, j).wait_send()
            for c in wb_copies(p, j):
                c.wait_send()
        for part in range(nr):
            fc_copy(p, part).wait_send()
        ss_copy(p).wait_send()
        da_copy(p).wait_send()

    each_f(drain)
    for j in range(1, nr):
        ps_copy(j).wait_send()
        pr_copy(j).wait_send()
        db_copy(j).wait_send()
    sq_copy.wait_send()
    for c in keep_w + [keep_f] + keep_d:
        c.wait()


def apply_kernel(
    nr, count, scale,
    fall_ref, wq_ref, wo_ref, dir_ref, proj_ref, sq_ref, w32q_ref, w32o_ref, fq_ref, fo_ref,
    m1q_ref, m2q_ref, m1o_ref, m2o_ref,
    nwq_ref, nwo_ref, sq_out, so_out, n1q_ref, n2q_ref, n1o_ref, n2o_ref, cq_ref, co_ref,
    dirs,
):
    ppa = nr // 2
    inverse = 1.0 / jnp.sqrt(sq_ref[0:1, 0:1] / count + 1e-06)

    @pl.when(pl.program_id(0) == 0)
    def _():
        dirs[0] = jnp.concatenate([dir_ref[q] for q in range(ppa)], axis=1)
        dirs[1] = jnp.concatenate([dir_ref[q] for q in range(ppa, nr)], axis=1).T
        step_q = jnp.dot(fq_ref[...], dirs[0], preferred_element_type=F32) * inverse
        sq_out[...] = step_q
        nwq_ref[...] = w32q_ref[...] - 0.01 * step_q
        step_o = nt_dot(dirs[1], fo_ref[...]) * inverse
        so_out[...] = step_o
        nwo_ref[...] = w32o_ref[...] - 0.01 * step_o
        proj_q = jnp.concatenate([proj_ref[q] for q in range(ppa)], axis=1).astype(F32) * scale
        proj_o = jnp.concatenate([proj_ref[q] for q in range(ppa, nr)], axis=1).astype(F32) * scale
        n1q_ref[...] = 0.8 * m1q_ref[...] + 0.2 * proj_q
        n2q_ref[...] = 0.9 * m2q_ref[...] + 0.1 * proj_q * proj_q
        n1o_ref[...] = 0.8 * m1o_ref[...] + 0.2 * proj_o
        n2o_ref[...] = 0.9 * m2o_ref[...] + 0.1 * proj_o * proj_o

    step_q = jnp.dot(fall_ref[0], dirs[0], preferred_element_type=F32) * inverse
    cq_ref[...] = (wq_ref[...].astype(F32) - 0.01 * step_q).astype(BF16)
    step_o = nt_dot(dirs[1], fall_ref[1]) * inverse
    whole_w = jnp.concatenate([wo_ref[m].astype(F32) for m in range(wo_ref.shape[0])], axis=1)
    co_ref[...] = (whole_w - 0.01 * step_o).astype(BF16)


def body(
    nf, nr,
    input_act, query_cot, out_cot, attn_out, query_w, out_w, query_factor, out_factor,
    first_q, second_q, first_o, second_o,
):
    tokens, d = input_act.shape
    hl = query_cot.shape[1]
    dl, rank = query_factor.shape
    rl = first_q.shape[0]
    pc = 2 * hl // nr
    scale = 1.0 / math.sqrt(tokens * nf * nr)
    anyspace = pl.BlockSpec(memory_space=pl.ANY)
    dma = pltpu.SemaphoreType.DMA
    sds = jax.ShapeDtypeStruct
    sems = []
    for shape in ((nf,), (nf, nr), (nf, nr), (nf, 2), (nf, nr, 2), (nr,), (nf,), (nr,), (nf,), (nr,), (1,)):
        sems += [dma(shape), dma(shape)]
    fall, wq_all, wo_all, dirs, projs, squares = pl.pallas_call(
        functools.partial(exchange_kernel, nf, nr, scale),
        out_shape=(
            sds((2, d, rank), BF16),
            sds((d, hl), BF16),
            sds((nf, hl, dl), BF16),
            sds((nr, rank, pc), BF16),
            sds((nr, rl, pc), BF16),
            sds((8, 128), F32),
        ),
        in_specs=[anyspace] * 12,
        out_specs=(anyspace,) * 5 + (pl.BlockSpec(memory_space=pltpu.VMEM),),
        scratch_shapes=[
            pltpu.VMEM((2, tokens, d), BF16),
            pltpu.VMEM((2, tokens, hl), BF16),
            pltpu.VMEM((hl, tokens), BF16),
            pltpu.VMEM((2, hl, d), BF16),
            pltpu.VMEM((2, d, rank), BF16),
            pltpu.VMEM((dl, hl), F32),
            pltpu.VMEM((hl, dl), F32),
            pltpu.VMEM((dl, hl), BF16),
            pltpu.VMEM((hl, dl), BF16),
            pltpu.VMEM((nr, rank, pc), BF16),
            pltpu.VMEM((nr, rank, pc), BF16),
            pltpu.VMEM((rank, pc), BF16),
            pltpu.VMEM((nf, rl, pc), BF16),
            pltpu.VMEM((2, rl, pc), F32),
            pltpu.VMEM((nr, rl, pc), BF16),
            pltpu.VMEM((nr, rank, pc), BF16),
            pltpu.VMEM((2, 8, pc), F32),
            dma((10,)),
        ] + sems,
        compiler_params=pltpu.CompilerParams(
            collective_id=0, has_side_effects=True, vmem_limit_bytes=48 * 1024 * 1024
        ),
    )(
        input_act, query_cot, out_cot, attn_out, query_w, out_w, query_factor, out_factor,
        first_q, second_q, first_o, second_o,
    )
    group = min(nf, max(1, 128 // dl))
    whole = lambda a: pl.BlockSpec(a.shape, lambda j, n=len(a.shape): (0,) * n)
    locals_in = (dirs, projs, squares, query_w, out_w, query_factor, out_factor, first_q, second_q, first_o, second_o)
    results = (query_w, out_w, query_w, out_w, first_q, second_q, first_o, second_o)
    outs = pl.pallas_call(
        functools.partial(apply_kernel, nr, 2 * rank * hl * 2, scale),
        grid=(nf // group,),
        out_shape=tuple(sds(a.shape, F32) for a in results) + (sds((d, hl), BF16), sds((hl, d), BF16)),
        in_specs=[
            pl.BlockSpec((2, group * dl, rank), lambda j: (0, j, 0)),
            pl.BlockSpec((group * dl, hl), lambda j: (j, 0)),
            pl.BlockSpec((group, hl, dl), lambda j: (j, 0, 0)),
        ] + [whole(a) for a in locals_in],
        out_specs=tuple(whole(a) for a in results) + (
            pl.BlockSpec((group * dl, hl), lambda j: (j, 0)),
            pl.BlockSpec((hl, group * dl), lambda j: (0, j)),
        ),
        scratch_shapes=[pltpu.VMEM((2, rank, hl), BF16)],
        compiler_params=pltpu.CompilerParams(vmem_limit_bytes=48 * 1024 * 1024),
    )(fall, wq_all, wo_all, *locals_in)
    return outs


def solution(mesh):
    return jax.shard_map(
        functools.partial(body, mesh.shape["fs"], mesh.shape["rep"]),
        mesh=mesh,
        in_specs=(
            P(("fs", "rep"), None),
            P(("fs", "rep"), "tp"),
            P(("fs", "rep"), None),
            P(("fs", "rep"), "tp"),
            P("fs", "tp"),
            P("tp", "fs"),
            P("fs", None),
            P("fs", None),
            P("fs", "tp"),
            P("fs", "tp"),
            P("fs", "tp"),
            P("fs", "tp"),
        ),
        out_specs=(
            P("fs", "tp"),
            P("tp", "fs"),
            P("fs", "tp"),
            P("tp", "fs"),
            P("fs", "tp"),
            P("fs", "tp"),
            P("fs", "tp"),
            P("fs", "tp"),
            P(None, "tp"),
            P("tp", None),
        ),
        check_vma=False,
    )
```

```python
import functools
import math

import jax
import jax.numpy as jnp
from jax import lax
from jax.experimental import pallas as pl
from jax.experimental.pallas import tpu as pltpu
from jax.sharding import PartitionSpec as P

MESH = pl.DeviceIdType.MESH
F32 = jnp.float32
BF16 = jnp.bfloat16


def rcopy(src, dst, sems, index, there, **where):
    return pltpu.make_async_remote_copy(
        src_ref=src,
        dst_ref=dst,
        send_sem=sems[0].at[index],
        recv_sem=sems[1].at[there],
        device_id=where,
        device_id_type=MESH,
    )


def nt_dot(a, b):
    return lax.dot_general(a, b, (((1,), (1,)), ((), ())), preferred_element_type=F32)


def exchange_kernel(
    nf, nr, scale,
    x_ref, cq_ref, y_ref, ca_ref, wq_ref, wo_ref, fq_ref, fo_ref, m1q_ref, m2q_ref, m1o_ref, m2o_ref,
    fall_out, wq_out, wo_out, dir_out, proj_out, sq_out,
    acts, cots, cot_t, grads, fall, w32q, w32o, wbq, wbo, pieces, piece_in, summed, summed_in,
    moms, proj_all, dir_all, sq_buf,
    loc, fa_s, fa_r, fb_s, fb_r, fc_s, fc_r, wa_s, wa_r, wb_s, wb_r, ps_s, ps_r, ss_s, ss_r,
    pr_s, pr_r, da_s, da_r, db_s, db_r, sq_s, sq_r,
):
    f, r, t = lax.axis_index("fs"), lax.axis_index("rep"), lax.axis_index("tp")
    ot = 1 - t
    dl, rank = fq_ref.shape
    hl = cq_ref.shape[1]
    dq, hd = dl // nr, hl // 2
    hq = (hl - hd) // nr
    rl = rank // nf
    pc = 2 * hl // nr
    ppa = nr // 2
    fa, fb, fc = (fa_s, fa_r), (fb_s, fb_r), (fc_s, fc_r)
    wa, wb = (wa_s, wa_r), (wb_s, wb_r)
    ps, ss, pr, da, db, sq = (ps_s, ps_r), (ss_s, ss_r), (pr_s, pr_r), (da_s, da_r), (db_s, db_r), (sq_s, sq_r)

    def fpeer(k):
        return lax.rem(f + k, nf)

    def rpeer(j):
        return lax.rem(r + j, nr)

    def each_f(body, first=1, last=nf):
        lax.fori_loop(first, last, lambda k, _: (body(k, fpeer(k)), 0)[1], 0)

    def rows(start, size):
        return pl.ds(pl.multiple_of(start, 16), size)

    def local(i, src, dst):
        return pltpu.make_async_copy(src, dst, loc.at[i])

    own_rows = rows(f * dl, dl)
    load_f = [local(0, fq_ref, fall.at[0, own_rows]), local(1, fo_ref, fall.at[1, own_rows])]
    load_w = [local(2, wq_ref, w32q), local(3, wo_ref, w32o)]
    load_c = [local(4, cq_ref, cots.at[0]), local(5, ca_ref, cots.at[1])]
    load_x = [local(6, x_ref, acts.at[0]), local(7, y_ref, acts.at[1])]
    for c in load_f + load_w + load_c + load_x:
        c.start()
    pcol = pl.ds(pl.multiple_of(lax.rem(r, ppa) * pc, pc), pc)

    @pl.when(r < ppa)
    def _():
        local(8, m1q_ref.at[:, pcol], moms.at[0]).start()
        local(9, m2q_ref.at[:, pcol], moms.at[1]).start()

    @pl.when(r >= ppa)
    def _():
        local(8, m1o_ref.at[:, pcol], moms.at[0]).start()
        local(9, m2o_ref.at[:, pcol], moms.at[1]).start()

    barrier = pltpu.get_barrier_semaphore()
    each_f(lambda k, p: pl.semaphore_signal(barrier, inc=1, device_id={"fs": p}, device_id_type=MESH))
    for j in range(1, nr):
        pl.semaphore_signal(barrier, inc=1, device_id={"rep": rpeer(j)}, device_id_type=MESH)
    pl.semaphore_signal(barrier, inc=1, device_id={"tp": ot}, device_id_type=MESH)
    pl.semaphore_wait(barrier, nf + nr - 1)

    def fchunk(core, block, part):
        ref = fall.at[core, rows(block * dl + part * dq, dq)]
        return ref

    def fa_copy(k, p):
        return rcopy(fchunk(t, f, r), fchunk(t, f, r), fa, p, f, fs=p)

    def fb_copy(p, j):
        return rcopy(fchunk(t, p, r), fchunk(t, p, r), fb, (p, rpeer(j)), (p, r), rep=rpeer(j))

    def fc_copy(p, part):
        return rcopy(fchunk(t, p, part), fchunk(t, p, part), fc, (p, part), (p, part), tp=ot)

    for c in load_f:
        c.wait()
    each_f(lambda k, p: fa_copy(k, p).start())

    for c in load_w:
        c.wait()
    wbq[...] = w32q[...].astype(BF16)
    wbo[...] = w32o[...].astype(BF16)
    keep_w = [local(2, wbq, wq_out.at[own_rows]), local(3, wbo, wo_out.at[f])]
    for c in keep_w:
        c.start()

    def wq_chunk(block):
        return wq_out.at[rows(block * dl + r * dq, dq)]

    def wo_chunk(block):
        return wo_out.at[block, rows(hd + r * hq, hq)]

    def wa_copies(p):
        return (
            rcopy(wbq.at[rows(r * dq, dq)], wq_chunk(f), wa, (p, 0), (f, 0), fs=p),
            rcopy(wbo.at[rows(hd + r * hq, hq)], wo_chunk(f), wa, (p, 1), (f, 1), fs=p),
        )

    def wd_copy(p):
        return rcopy(wbo.at[pl.ds(0, hd)], wo_out.at[f, pl.ds(0, hd)], wa, (p, 2), (f, 2), fs=p)

    def wd_recv(p):
        return rcopy(wbo.at[pl.ds(0, hd)], wo_out.at[p, pl.ds(0, hd)], wa, (p, 2), (p, 2), fs=p)

    def wa_recv(p):
        return (
            rcopy(wbq.at[rows(r * dq, dq)], wq_chunk(p), wa, (p, 0), (p, 0), fs=p),
            rcopy(wbo.at[rows(hd + r * hq, hq)], wo_chunk(p), wa, (p, 1), (p, 1), fs=p),
        )

    def wb_copies(p, j):
        q = rpeer(j)
        return (
            rcopy(wq_chunk(p), wq_chunk(p), wb, (p, q, 0), (p, r, 0), rep=q),
            rcopy(wo_chunk(p), wo_chunk(p), wb, (p, q, 1), (p, r, 1), rep=q),
        )

    def wb_recv(p, j):
        q = rpeer(j)
        there_q = wq_out.at[rows(p * dl + q * dq, dq)]
        there_o = wo_out.at[p, rows(hd + q * hq, hq)]
        return (
            rcopy(there_q, there_q, wb, (p, q, 0), (p, q, 0), rep=q),
            rcopy(there_o, there_o, wb, (p, q, 1), (p, q, 1), rep=q),
        )

    def start_all(copies):
        for c in copies:
            c.start()

    each_f(lambda k, p: wa_copies(p)[0].start())
    each_f(lambda k, p: wa_copies(p)[1].start())
    each_f(lambda k, p: wd_copy(p).start())

    nb = min(512, x_ref.shape[1])

    def gradient(i):
        load_c[i].wait()
        cot_t[...] = cots[i].T
        load_x[i].wait()

        def column(n, _):
            cols = pl.ds(pl.multiple_of(n * nb, nb), nb)
            grads[i, :, cols] = jnp.dot(cot_t[...], acts[i, :, cols], preferred_element_type=F32).astype(BF16)
            return 0

        lax.fori_loop(0, x_ref.shape[1] // nb, column, 0)

    def forward_f(k, p):
        rcopy(fchunk(t, p, r), fchunk(t, p, r), fa, p, p, fs=p).wait_recv()
        for j in range(1, nr):
            fb_copy(p, j).start()
        fc_copy(p, r).start()

    early = 1 + (nf - 1) // 3
    each_f(forward_f, 1, early)
    gradient(0)
    each_f(forward_f, early, nf)
    gradient(1)

    def across_f(k, p):
        for j in range(1, nr):
            q = rpeer(j)
            rcopy(fchunk(t, p, q), fchunk(t, p, q), fb, (p, q), (p, q), rep=q).wait_recv()
            fc_copy(p, q).start()

    each_f(across_f)

    def rest_f(k, p):
        for part in range(nr):
            rcopy(fchunk(ot, p, part), fchunk(ot, p, part), fc, (p, part), (p, part), tp=ot).wait_recv()

    each_f(rest_f)
    keep_f = local(0, fall, fall_out)
    keep_f.start()

    def forward_w(which):
        def step(k, p):
            wa_recv(p)[which].wait_recv()
            for j in range(1, nr):
                wb_copies(p, j)[which].start()

        each_f(step)

    forward_w(0)

    rb = min(256, rank)
    for i in range(2):
        def ranks(n, _, i=i):
            cols = pl.ds(pl.multiple_of(n * rb, rb), rb)
            term = jnp.dot(grads[i], fall[i, :, cols], preferred_element_type=F32).T.astype(BF16)
            for part in range(ppa):
                pieces[i * ppa + part, cols, :] = term[:, part * pc:(part + 1) * pc]
            return 0

        lax.fori_loop(0, rank // rb, ranks, 0)

    def ps_copy(j):
        q = rpeer(j)
        return rcopy(pieces.at[q], piece_in.at[r], ps, q, r, rep=q)

    for j in range(1, nr):
        ps_copy(j).start()

    for j in range(1, nr):
        q = rpeer(j)
        rcopy(pieces.at[q], piece_in.at[q], ps, q, q, rep=q).wait_recv()
    total = pieces[r].astype(F32)
    for j in range(1, nr):
        total = total + piece_in[rpeer(j)].astype(F32)
    summed[...] = total.astype(BF16)

    def ss_copy(p):
        return rcopy(summed.at[rows(p * rl, rl)], summed_in.at[f], ss, p, f, fs=p)

    each_f(lambda k, p: ss_copy(p).start())
    forward_w(1)

    own_rank = rows(f * rl, rl)

    def gather_sum(k, total):
        p = fpeer(k)
        rcopy(summed.at[own_rank], summed_in.at[p], ss, p, p, fs=p).wait_recv()
        return total + summed_in[p].astype(F32)

    proj = lax.fori_loop(1, nf, gather_sum, summed[own_rank, :].astype(F32)).astype(BF16)
    proj_all[r] = proj

    def pr_copy(j):
        q = rpeer(j)
        return rcopy(proj_all.at[r], proj_all.at[r], pr, q, r, rep=q)

    proj = proj.astype(F32) * scale
    local(8, m1q_ref.at[:, pcol], moms.at[0]).wait()
    local(9, m2q_ref.at[:, pcol], moms.at[1]).wait()
    first = 0.8 * moms[0] + 0.2 * proj
    second = 0.9 * moms[1] + 0.1 * proj * proj
    dir_all[r, own_rank, :] = (first / jnp.sqrt(second)).astype(BF16)

    def da_copy(p):
        return rcopy(dir_all.at[r, own_rank], dir_all.at[r, own_rank], da, p, f, fs=p)

    each_f(lambda k, p: da_copy(p).start())
    for j in range(1, nr):
        pr_copy(j).start()

    def da_wait(k, p):
        there = dir_all.at[r, rows(p * rl, rl)]
        rcopy(there, there, da, p, p, fs=p).wait_recv()

    each_f(da_wait)

    def db_copy(j):
        q = rpeer(j)
        return rcopy(dir_all.at[r], dir_all.at[r], db, q, r, rep=q)

    for j in range(1, nr):
        db_copy(j).start()
    for j in range(1, nr):
        q = rpeer(j)
        rcopy(dir_all.at[q], dir_all.at[q], db, q, q, rep=q).wait_recv()
        rcopy(proj_all.at[q], proj_all.at[q], pr, q, q, rep=q).wait_recv()
    keep_d = [local(4, dir_all, dir_out), local(5, proj_all, proj_out)]
    start_all(keep_d)

    squares = jnp.zeros((8, pc), F32)
    for q in range(nr):
        d = dir_all[q].astype(F32)
        squares = squares + jnp.sum((d * d).reshape(rank // 8, 8, pc), axis=0)
    sq_buf[0] = squares
    sq_copy = rcopy(sq_buf.at[0], sq_buf.at[1], sq, 0, 0, tp=ot)
    sq_copy.start()
    sq_copy.wait_recv()
    sq_out[...] = jnp.zeros(sq_out.shape, F32) + jnp.sum(sq_buf[0] + sq_buf[1])

    def rest_w(k, p):
        wd_recv(p).wait_recv()
        for j in range(1, nr):
            for c in wb_recv(p, j):
                c.wait_recv()

    each_f(rest_w)

    def drain(k, p):
        fa_copy(k, p).wait_send()
        for c in wa_copies(p):
            c.wait_send()
        wd_copy(p).wait_send()
        for j in range(1, nr):
            fb_copy(p, j).wait_send()
            for c in wb_copies(p, j):
                c.wait_send()
        for part in range(nr):
            fc_copy(p, part).wait_send()
        ss_copy(p).wait_send()
        da_copy(p).wait_send()

    each_f(drain)
    for j in range(1, nr):
        ps_copy(j).wait_send()
        pr_copy(j).wait_send()
        db_copy(j).wait_send()
    sq_copy.wait_send()
    for c in keep_w + [keep_f] + keep_d:
        c.wait()


def apply_kernel(
    nr, count, scale,
    fall_ref, wq_ref, wo_ref, dir_ref, proj_ref, sq_ref, w32q_ref, w32o_ref, fq_ref, fo_ref,
    m1q_ref, m2q_ref, m1o_ref, m2o_ref,
    nwq_ref, nwo_ref, sq_out, so_out, n1q_ref, n2q_ref, n1o_ref, n2o_ref, cq_ref, co_ref,
    dirs,
):
    ppa = nr // 2
    inverse = 1.0 / jnp.sqrt(sq_ref[0:1, 0:1] / count + 1e-06)

    @pl.when(pl.program_id(0) == 0)
    def _():
        dirs[0] = jnp.concatenate([dir_ref[q] for q in range(ppa)], axis=1)
        dirs[1] = jnp.concatenate([dir_ref[q] for q in range(ppa, nr)], axis=1).T
        step_q = jnp.dot(fq_ref[...], dirs[0], preferred_element_type=F32) * inverse
        sq_out[...] = step_q
        nwq_ref[...] = w32q_ref[...] - 0.01 * step_q
        step_o = nt_dot(dirs[1], fo_ref[...]) * inverse
        so_out[...] = step_o
        nwo_ref[...] = w32o_ref[...] - 0.01 * step_o
        proj_q = jnp.concatenate([proj_ref[q] for q in range(ppa)], axis=1).astype(F32) * scale
        proj_o = jnp.concatenate([proj_ref[q] for q in range(ppa, nr)], axis=1).astype(F32) * scale
        n1q_ref[...] = 0.8 * m1q_ref[...] + 0.2 * proj_q
        n2q_ref[...] = 0.9 * m2q_ref[...] + 0.1 * proj_q * proj_q
        n1o_ref[...] = 0.8 * m1o_ref[...] + 0.2 * proj_o
        n2o_ref[...] = 0.9 * m2o_ref[...] + 0.1 * proj_o * proj_o

    step_q = jnp.dot(fall_ref[0], dirs[0], preferred_element_type=F32) * inverse
    cq_ref[...] = (wq_ref[...].astype(F32) - 0.01 * step_q).astype(BF16)
    step_o = nt_dot(dirs[1], fall_ref[1]) * inverse
    whole_w = jnp.concatenate([wo_ref[m].astype(F32) for m in range(wo_ref.shape[0])], axis=1)
    co_ref[...] = (whole_w - 0.01 * step_o).astype(BF16)


def body(
    nf, nr,
    input_act, query_cot, out_cot, attn_out, query_w, out_w, query_factor, out_factor,
    first_q, second_q, first_o, second_o,
):
    tokens, d = input_act.shape
    hl = query_cot.shape[1]
    dl, rank = query_factor.shape
    rl = first_q.shape[0]
    pc = 2 * hl // nr
    scale = 1.0 / math.sqrt(tokens * nf * nr)
    anyspace = pl.BlockSpec(memory_space=pltpu.HBM)
    dma = pltpu.SemaphoreType.DMA
    sds = jax.ShapeDtypeStruct
    sems = []
    for shape in ((nf,), (nf, nr), (nf, nr), (nf, 3), (nf, nr, 2), (nr,), (nf,), (nr,), (nf,), (nr,), (1,)):
        sems += [dma(shape), dma(shape)]
    fall, wq_all, wo_all, dirs, projs, squares = pl.pallas_call(
        functools.partial(exchange_kernel, nf, nr, scale),
        out_shape=(
            sds((2, d, rank), BF16),
            sds((d, hl), BF16),
            sds((nf, hl, dl), BF16),
            sds((nr, rank, pc), BF16),
            sds((nr, rl, pc), BF16),
            sds((8, 128), F32),
        ),
        in_specs=[anyspace] * 12,
        out_specs=(anyspace,) * 5 + (pl.BlockSpec(memory_space=pltpu.VMEM),),
        scratch_shapes=[
            pltpu.VMEM((2, tokens, d), BF16),
            pltpu.VMEM((2, tokens, hl), BF16),
            pltpu.VMEM((hl, tokens), BF16),
            pltpu.VMEM((2, hl, d), BF16),
            pltpu.VMEM((2, d, rank), BF16),
            pltpu.VMEM((dl, hl), F32),
            pltpu.VMEM((hl, dl), F32),
            pltpu.VMEM((dl, hl), BF16),
            pltpu.VMEM((hl, dl), BF16),
            pltpu.VMEM((nr, rank, pc), BF16),
            pltpu.VMEM((nr, rank, pc), BF16),
            pltpu.VMEM((rank, pc), BF16),
            pltpu.VMEM((nf, rl, pc), BF16),
            pltpu.VMEM((2, rl, pc), F32),
            pltpu.VMEM((nr, rl, pc), BF16),
            pltpu.VMEM((nr, rank, pc), BF16),
            pltpu.VMEM((2, 8, pc), F32),
            dma((10,)),
        ] + sems,
        compiler_params=pltpu.CompilerParams(
            collective_id=0, has_side_effects=True, vmem_limit_bytes=67043328
        ),
    )(
        input_act, query_cot, out_cot, attn_out, query_w, out_w, query_factor, out_factor,
        first_q, second_q, first_o, second_o,
    )
    group = min(nf, max(1, 128 // dl))
    whole = lambda a: pl.BlockSpec(a.shape, lambda j, n=len(a.shape): (0,) * n)
    locals_in = (dirs, projs, squares, query_w, out_w, query_factor, out_factor, first_q, second_q, first_o, second_o)
    results = (query_w, out_w, query_w, out_w, first_q, second_q, first_o, second_o)
    outs = pl.pallas_call(
        functools.partial(apply_kernel, nr, 2 * rank * hl * 2, scale),
        grid=(nf // group,),
        out_shape=tuple(sds(a.shape, F32) for a in results) + (sds((d, hl), BF16), sds((hl, d), BF16)),
        in_specs=[
            pl.BlockSpec((2, group * dl, rank), lambda j: (0, j, 0)),
            pl.BlockSpec((group * dl, hl), lambda j: (j, 0)),
            pl.BlockSpec((group, hl, dl), lambda j: (j, 0, 0)),
        ] + [whole(a) for a in locals_in],
        out_specs=tuple(whole(a) for a in results) + (
            pl.BlockSpec((group * dl, hl), lambda j: (j, 0)),
            pl.BlockSpec((hl, group * dl), lambda j: (0, j)),
        ),
        scratch_shapes=[pltpu.VMEM((2, rank, hl), BF16)],
        compiler_params=pltpu.CompilerParams(vmem_limit_bytes=67043328),
    )(fall, wq_all, wo_all, *locals_in)
    return outs


def solution(mesh):
    return jax.shard_map(
        functools.partial(body, mesh.shape["fs"], mesh.shape["rep"]),
        mesh=mesh,
        in_specs=(
            P(("fs", "rep"), None),
            P(("fs", "rep"), "tp"),
            P(("fs", "rep"), None),
            P(("fs", "rep"), "tp"),
            P("fs", "tp"),
            P("tp", "fs"),
            P("fs", None),
            P("fs", None),
            P("fs", "tp"),
            P("fs", "tp"),
            P("fs", "tp"),
            P("fs", "tp"),
        ),
        out_specs=(
            P("fs", "tp"),
            P("tp", "fs"),
            P("fs", "tp"),
            P("tp", "fs"),
            P("fs", "tp"),
            P("fs", "tp"),
            P("fs", "tp"),
            P("fs", "tp"),
            P(None, "tp"),
            P("tp", None),
        ),
        check_vma=False,
    )
```
